256 devices in a mesh: fs: 32 (over z, y), tp: 8 (over x, core).
Axes of the slice: x: 4, y: 4, z: 8, core: 2. Of those that a mesh axis runs over, the one named last changes fastest.
Arguments:
- tokens: bfloat16 [32768, 2048], P(('fs', 'tp')), may hold values from -6 to 6
- pre_gain: float32 [2048], replicated, may hold values from 0.1 to 1.9
- w_expand: bfloat16 [2048, 8192], P('fs', 'tp'), may hold values from -0.125 to 0.125
- w_reduce: bfloat16 [8192, 2048], P('tp', 'fs'), may hold values from -0.0625 to 0.0625
- post_gain: float32 [2048], replicated, may hold values from 0.1 to 1.9
Outputs:
- result: bfloat16 [32768, 2048], P(('fs', 'tp'))
The draws below stay inside these ranges and needn't reach their ends.
All inputs are finite; a program needn't handle non-finite values.
Results may differ from the reference program's by a relative error of at most 0.014.
Values may be sent and summed in bfloat16 or wider, within the bound.
No kernel may reach another device: no remote copies, remote signals or barrier semaphores. Data moves between devices by JAX's collectives and lax.ppermute only.
A program may use at most 64 MiB of HBM per device.

```python
import math
import jax
import jax.numpy as jnp
from jax import lax

D = 2048
FF = 8192
TOKENS = 32768
N_TP = 8


def block_levels(key, shape, cuts, low, top_value):
    level, own = 1.0, jax.random.fold_in(key, 6)
    for dim, parts in cuts:
        draws = jnp.exp(jax.random.uniform(jax.random.fold_in(own, dim), (parts,), jnp.float32, low / len(cuts), top_value / len(cuts)))
        level = level * jnp.repeat(draws, shape[dim] // parts).reshape([-1 if axis == dim else 1 for axis in range(len(shape))])
    return level


def centred(key, extent, deviation, reach, shards=(), held_as=jnp.bfloat16):
    drawn = jax.random.normal(key, extent, jnp.float32) * deviation
    if len(shards) > 0:
        drawn = block_levels(key, extent, shards, -0.22, 0.18) * drawn
    return jnp.clip(drawn, min=-reach, max=reach).astype(held_as)


def setup_inputs(seed: int = 0) -> dict:
    key_list = jax.random.split(jax.random.key(seed), 6)
    return {
        "tokens": centred(key_list[0], (TOKENS, D), 1.0, 6.0, ((0, 256),)),
        "pre_gain": jnp.clip(1.0 + 0.18 * jax.random.normal(key_list[1], (D,), jnp.float32), 0.1, 1.9),
        "w_expand": centred(key_list[2], (D, FF), D ** -0.5, 0.125, ((0, 32), (1, 8))),
        "w_reduce": centred(key_list[3], (FF, D), FF ** -0.5, 0.0625, ((0, 8), (1, 32))),
        "post_gain": jnp.clip(1.0 + 0.18 * jax.random.normal(key_list[4], (D,), jnp.float32), 0.1, 1.9),
    }


NORM_EPS = 1e-06

def rms_scale(values, gain_row):
    widened = values.astype(jnp.float32)
    scaled = widened * lax.rsqrt(lax.optimization_barrier(jnp.mean(widened * widened, axis=-1, keepdims=True)) + NORM_EPS)
    return scaled * gain_row.astype(jnp.float32)

def reference(tokens, pre_gain, w_expand, w_reduce, post_gain):
    row_count = tokens.shape[0]
    block_rows = math.gcd(row_count, 2048)
    blocks = tokens.reshape(row_count // block_rows, block_rows, D)
    hidden_block = FF // N_TP

    def per_block(block):
        normed = rms_scale(block, pre_gain).astype(jnp.bfloat16)
        preact = jnp.dot(normed, w_expand, preferred_element_type=jnp.float32)
        hidden = jnp.square(jnp.maximum(preact, 0.0)).astype(jnp.bfloat16)
        running = jnp.zeros((block_rows, D), jnp.float32)
        for member in range(N_TP):
            partial_value = jnp.dot(hidden[:, member * hidden_block:(member + 1) * hidden_block], w_reduce[member * hidden_block:(member + 1) * hidden_block], preferred_element_type=jnp.float32).astype(jnp.bfloat16)
            partial_value = lax.optimization_barrier(partial_value)
            running = running + partial_value.astype(jnp.float32)
        mixed = running.astype(jnp.bfloat16)
        return rms_scale(mixed, post_gain).astype(jnp.bfloat16)
    return lax.map(per_block, blocks).reshape(row_count, D)
```

```python
import jax
import jax.numpy as jnp
from jax import lax
from jax.experimental import pallas as pl
from jax.experimental.pallas import tpu as pltpu
from jax.sharding import PartitionSpec as P

NORM_EPS = 1e-06
NZ, NY, NX = 8, 4, 4
AXES = ("fs", "tp")


def flat(z, y, x, c):
    return ((z % NZ) * NY + y % NY) * (2 * NX) + (x % NX) * 2 + c


def moves(step):
    return [
        (flat(z, y, x, c), flat(*step(z, y, x, c)))
        for z in range(NZ)
        for y in range(NY)
        for x in range(NX)
        for c in range(2)
    ]


def send_z(a, d):
    return lax.ppermute(a, AXES, moves(lambda z, y, x, c: (z + (d if c == 0 else -d), y, x, c)))


def send_y(a, d):
    return lax.ppermute(a, AXES, moves(lambda z, y, x, c: (z, y + (d if c == 0 else -d), x, c)))


def send_x(a, d):
    return lax.ppermute(a, AXES, moves(lambda z, y, x, c: (z, y, x + d, c)))


def swap(a):
    return lax.ppermute(a, AXES, moves(lambda z, y, x, c: (z, y, x, 1 - c)))


def place():
    fs, tp = lax.axis_index("fs"), lax.axis_index("tp")
    return fs // NY, fs % NY, tp % 2


ROWS = 16
UNIT = 256


def unit_at(k):
    return pl.ds(pl.multiple_of(lax.rem(k, NZ) * UNIT, UNIT), UNIT)


def norm_body(where_ref, x_ref, gain_ref, out_ref):
    def step(i, _):
        rows = pl.ds(pl.multiple_of(i * ROWS, ROWS), ROWS)
        x = x_ref[rows, :].astype(jnp.float32)
        scale = lax.rsqrt(jnp.mean(x * x, axis=-1, keepdims=True) + NORM_EPS)
        y = (x * scale) * gain_ref[...]
        turn = lax.rem(NY - where_ref[1], NY) * (UNIT // NY)
        for k in range(NZ):
            unit = pltpu.roll(y[:, UNIT * k : UNIT * (k + 1)], turn, 1)
            out_ref[rows, unit_at(k + NZ - where_ref[0])] = unit.astype(jnp.bfloat16)
        return 0

    lax.fori_loop(0, x_ref.shape[0] // ROWS, step, 0)


def pre_norm(where, tokens, gain):
    cost = pl.CostEstimate(flops=8 << 20, bytes_accessed=1 << 20, transcendentals=128)
    out = jax.ShapeDtypeStruct(tokens.shape, jnp.bfloat16)
    args = [where, tokens, gain.reshape(1, -1)]
    return vmem_call(norm_body, out, args, limit=4 << 20, scalars=1, cost_estimate=cost)


def last_body(where_ref, *refs):
    parts, gain_ref, out_ref = refs[:-2], refs[-2], refs[-1]

    def step(i, _):
        rows = pl.ds(pl.multiple_of(i * ROWS, ROWS), ROWS)
        total = parts[0][rows, :].astype(jnp.float32)
        for p in parts[1:]:
            total += p[rows, :].astype(jnp.float32)
        x = total.astype(jnp.bfloat16).astype(jnp.float32)
        y = x * lax.rsqrt(jnp.mean(x * x, axis=-1, keepdims=True) + NORM_EPS)
        turn = where_ref[1] * (UNIT // NY)
        for k in range(NZ):
            unit = pltpu.roll(y[:, UNIT * k : UNIT * (k + 1)], turn, 1)
            there = unit_at(k + where_ref[0])
            out_ref[rows, there] = (unit * gain_ref[:, there]).astype(jnp.bfloat16)
        return 0

    lax.fori_loop(0, out_ref.shape[0] // ROWS, step, 0)


def last_norm(where, parts, gain):
    out = jax.ShapeDtypeStruct((parts[0].shape[0], gain.shape[0]), jnp.bfloat16)
    args = [where, *parts, gain.reshape(1, -1)]
    return vmem_call(last_body, out, args, limit=6 << 20, scalars=1)


def mark(where):
    def body(in_ref, out_ref):
        for k in range(3):
            out_ref[k] = in_ref[k]

    spec = pl.BlockSpec(memory_space=pltpu.SMEM)
    return pl.pallas_call(
        body,
        out_shape=jax.ShapeDtypeStruct(where.shape, where.dtype),
        in_specs=[spec],
        out_specs=spec,
        compiler_params=pltpu.CompilerParams(vmem_limit_bytes=1 << 20),
    )(where)


def vmem_call(body, outs, args, limit, scalars=0, **kw):
    return pl.pallas_call(
        body,
        out_shape=outs,
        in_specs=[pl.BlockSpec(memory_space=pltpu.SMEM)] * scalars
        + [pl.BlockSpec(memory_space=pltpu.VMEM)] * (len(args) - scalars),
        out_specs=jax.tree.map(lambda _: pl.BlockSpec(memory_space=pltpu.VMEM), outs),
        compiler_params=pltpu.CompilerParams(vmem_limit_bytes=limit),
        **kw,
    )(*args)


def ring_units(where, own, pieces, theirs):
    steps = len(pieces)
    count, rows = 2 * steps, own.shape[0] // 2
    part = rows // 2

    def body(where_ref, own_ref, *refs):
        others, outs = refs[steps], refs[steps + 1 :]

        def mine(k, start, size):
            return refs[k][pl.ds(start, size), :]

        def other(k, start, size):
            return others[pl.ds(k * 2 * rows + start, size), :]

        def put(low, high):
            for w, out in enumerate(outs):
                out[pl.ds(0, rows), :] = own_ref[pl.ds(w * rows, rows), :]
                for k in range(1, steps):
                    out[pl.ds(k * rows, rows), :] = high(k - 1, w * rows, rows)
                    out[pl.ds((count - k) * rows, rows), :] = low(k - 1, w * rows, rows)
                out[pl.ds(steps * rows, part), :] = low(steps - 1, w * part, part)
                out[pl.ds(steps * rows + part, part), :] = high(steps - 1, w * part, part)

        pl.when(where_ref[2] == 0)(lambda: put(mine, other))
        pl.when(where_ref[2] == 1)(lambda: put(other, mine))

    unit = jax.ShapeDtypeStruct((count * rows, own.shape[1]), own.dtype)
    size = 2 * (own.size * (count + 1) * 2)
    cost = pl.CostEstimate(flops=1 << 20, bytes_accessed=size, transcendentals=0)
    return vmem_call(
        body, [unit, unit], [where, own, *pieces, theirs], limit=size + (1 << 20), scalars=1, cost_estimate=cost
    )


def layer(tokens, pre_gain, w_expand, w_reduce, post_gain):
    z, y, core = place()
    first = core == 0
    where = jnp.stack([z, y, core]).astype(jnp.int32)

    def low_high(mine, theirs):
        return jnp.where(first, mine, theirs), jnp.where(first, theirs, mine)

    def half(a):
        n = a.shape[0] // 2
        return jnp.where(first, a[:n], a[n:])

    def half_pair(a):
        n = a.shape[0] // 4
        return jnp.concatenate([jnp.where(first, a[k : k + n], a[k + n : k + 2 * n]) for k in (0, 2 * n)], 0)

    def ring(pieces, theirs):
        lows, highs = zip(*(low_high(a, b) for a, b in zip(pieces, theirs)))
        return list(highs[:-1]) + [jnp.concatenate([lows[-1], highs[-1]], 0)] + list(lows[:-1][::-1])

    mine = jnp.concatenate([w_expand, w_reduce.T], 0)
    other = swap(mine)
    normed = pre_norm(where, tokens, pre_gain)
    block0, block1 = low_high(mine, other)
    z1, z2 = send_z(block0, 1), send_z(block0, 2)
    y1, y2 = send_y(block1, 1), send_y(half_pair(block1), 2)
    everyone = jnp.concatenate([normed, send_x(normed, -1), send_x(normed, 2), send_x(normed, 1)], 0)
    ys = swap(jnp.concatenate([y1, y2], 0))
    ve, vr = ring_units(where, block1, [y1, y2], ys)
    z3, z4 = send_z(z2, 1), send_z(half_pair(z2), 2)
    zs = swap(jnp.concatenate([z1, z2, z3, z4], 0))
    ue, ur = ring_units(where, block0, [z1, z2, z3, z4], zs)

    def heavy_z(unit):
        v, got = unit, []
        for k in range(4):
            v = send_z(half(v) if k == 3 else v, 1)
            got.append(v)
        return got, swap(jnp.concatenate(got[2:], 0))

    def heavy_y(unit, together):
        u1 = send_y(unit, 1)
        u2 = send_y(half(u1), 1)
        rows = u1.shape[0]
        if together:
            both = swap(jnp.concatenate([u1, u2], 0))
            theirs = [both[:rows], both[rows:]]
        else:
            theirs = [swap(u1), swap(u2)]
        units = [unit] + ring([u1, u2], theirs)
        return jnp.stack([u.reshape(NZ, u.shape[0] // NZ, -1) for u in units], 1)

    (ge, se), (gr, sr) = heavy_z(ve), heavy_z(vr)
    near = swap(jnp.concatenate(ge[:2] + gr[:2], 0))
    rows = ve.shape[0]
    e1 = [ve] + ring(ge, [near[:rows], near[rows : 2 * rows], se[:rows], se[rows:]])
    r1 = [vr] + ring(gr, [near[2 * rows : 3 * rows], near[3 * rows :], sr[:rows], sr[rows:]])
    e0, r0 = heavy_y(ue, True), heavy_y(ur, False)

    def expand(w):
        pre = jnp.dot(everyone, w, preferred_element_type=jnp.float32)
        return jnp.square(jnp.maximum(pre, 0.0)).astype(jnp.bfloat16)

    h1 = expand(jnp.concatenate(e1, 0))
    h0 = expand(e0.reshape(-1, e0.shape[-1]))
    hidden = jnp.concatenate([h0, h1], 1)
    tn = (((1,), (1,)), ((), ()))
    weights = jnp.concatenate([r0.reshape(-1, r0.shape[-1]), jnp.concatenate(r1, 0)], 1)
    rows = tokens.shape[0]

    def mix(a, w):
        return lax.dot_general(a, w, tn, preferred_element_type=jnp.float32).astype(jnp.bfloat16)

    later = mix(hidden[: 2 * rows], weights)
    first = mix(hidden[2 * rows :], weights)
    m = [later[:rows], later[rows:], first[:rows], first[rows:]]
    p2, p3 = send_x(m[2], 2), send_x(m[3], -1)
    parts = [m[0], send_x(m[1], 1), p2, p3]
    return last_norm(mark(where), parts, post_gain)


def solution(mesh):
    return jax.shard_map(
        layer,
        mesh=mesh,
        in_specs=(P(("fs", "tp"), None), P(), P("fs", "tp"), P("tp", "fs"), P()),
        out_specs=P(("fs", "tp"), None),
        check_vma=False,
    )
```

```python
import jax
import jax.numpy as jnp
from jax import lax
from jax.experimental import pallas as pl
from jax.experimental.pallas import tpu as pltpu
from jax.sharding import PartitionSpec as P

NORM_EPS = 1e-06
NZ, NY, NX = 8, 4, 4
AXES = ("fs", "tp")


def flat(z, y, x, c):
    return ((z % NZ) * NY + y % NY) * (2 * NX) + (x % NX) * 2 + c


def moves(step):
    return [
        (flat(z, y, x, c), flat(*step(z, y, x, c)))
        for z in range(NZ)
        for y in range(NY)
        for x in range(NX)
        for c in range(2)
    ]


def send_z(a, d):
    return lax.ppermute(a, AXES, moves(lambda z, y, x, c: (z + (d if c == 0 else -d), y, x, c)))


def send_y(a, d):
    return lax.ppermute(a, AXES, moves(lambda z, y, x, c: (z, y + (d if c == 0 else -d), x, c)))


def send_x(a, d):
    return lax.ppermute(a, AXES, moves(lambda z, y, x, c: (z, y, x + d, c)))


def swap(a):
    return lax.ppermute(a, AXES, moves(lambda z, y, x, c: (z, y, x, 1 - c)))


def place():
    fs, tp = lax.axis_index("fs"), lax.axis_index("tp")
    return fs // NY, fs % NY, tp % 2


ROWS = 16
UNIT = 256


def unit_at(k):
    return pl.ds(pl.multiple_of(lax.rem(k, NZ) * UNIT, UNIT), UNIT)


def norm_body(where_ref, x_ref, gain_ref, out_ref):
    def step(i, _):
        rows = pl.ds(pl.multiple_of(i * ROWS, ROWS), ROWS)
        x = x_ref[rows, :].astype(jnp.float32)
        scale = lax.rsqrt(jnp.mean(x * x, axis=-1, keepdims=True) + NORM_EPS)
        y = (x * scale) * gain_ref[...]
        turn = lax.rem(NY - where_ref[1], NY) * (UNIT // NY)
        for k in range(NZ):
            unit = pltpu.roll(y[:, UNIT * k : UNIT * (k + 1)], turn, 1)
            out_ref[rows, unit_at(k + NZ - where_ref[0])] = unit.astype(jnp.bfloat16)
        return 0

    lax.fori_loop(0, x_ref.shape[0] // ROWS, step, 0)


def pre_norm(where, tokens, gain):
    cost = pl.CostEstimate(flops=8 << 20, bytes_accessed=1 << 20, transcendentals=128)
    out = jax.ShapeDtypeStruct(tokens.shape, jnp.bfloat16)
    args = [where, tokens, gain.reshape(1, -1)]
    return vmem_call(norm_body, out, args, limit=4 << 20, scalars=1, cost_estimate=cost)


def last_body(groups, where_ref, *refs):
    parts, gain_ref, out_ref = refs[:-2], refs[-2], refs[-1]
    size = len(parts) // groups
    block = 4 * ROWS

    def step(i, _):
        rows = pl.ds(pl.multiple_of(i * block, block), block)
        sums = []
        for g in range(groups):
            total = parts[g * size][rows, :].astype(jnp.float32)
            for p in parts[g * size + 1 : (g + 1) * size]:
                total += p[rows, :].astype(jnp.float32)
            sums.append(total.astype(jnp.bfloat16).astype(jnp.float32))
        square = sum(jnp.sum(x * x, axis=-1, keepdims=True) for x in sums)
        scale = lax.rsqrt(square / out_ref.shape[1] + NORM_EPS)
        x = jnp.concatenate(sums, axis=1) * scale

        def cut(z, y, n=1):
            at = CHUNK * chunk_at(z, y)
            return x[:, at : at + n * CHUNK]

        turn = where_ref[1] * (UNIT // NY)
        for k in range(NZ):
            unit = jnp.concatenate([cut(k, 0, 2), cut(k, 2), cut(k, 3)], axis=1)
            unit = pltpu.roll(unit, turn, 1)
            there = unit_at(k + where_ref[0])
            out_ref[rows, there] = (unit * gain_ref[:, there]).astype(jnp.bfloat16)
        return 0

    lax.fori_loop(0, out_ref.shape[0] // block, step, 0)


def chunk_at(z, y):
    near = z < 3 or z > 5
    order = z - 3 if z > 5 else z
    if y < 2:
        return 2 * order + y if near else EARLY + 12 + 2 * (z - 3) + y
    if y == 2:
        return EARLY + z
    return 10 + order - 1 if near and z != 0 else EARLY + 8 + (z - 2 if z else 0)


def last_norm(where, groups, gain):
    parts = [p for g in groups for p in g]
    out = jax.ShapeDtypeStruct((parts[0].shape[0], gain.shape[0]), jnp.bfloat16)

    def body(*refs):
        last_body(len(groups), *refs)

    args = [where, *parts, gain.reshape(1, -1)]
    return vmem_call(body, out, args, limit=6 << 20, scalars=1)


def vmem_call(body, outs, args, limit, scalars=0, **kw):
    return pl.pallas_call(
        body,
        out_shape=outs,
        in_specs=[pl.BlockSpec(memory_space=pltpu.SMEM)] * scalars
        + [pl.BlockSpec(memory_space=pltpu.VMEM)] * (len(args) - scalars),
        out_specs=jax.tree.map(lambda _: pl.BlockSpec(memory_space=pltpu.VMEM), outs),
        compiler_params=pltpu.CompilerParams(vmem_limit_bytes=limit),
        **kw,
    )(*args)


def ring_units(where, own, pieces, theirs):
    steps = len(pieces)
    count, rows = 2 * steps, own.shape[0] // 2
    part = rows // 2

    def body(where_ref, own_ref, *refs):
        others, outs = refs[steps], refs[steps + 1 :]

        def mine(k, start, size):
            return refs[k][pl.ds(start, size), :]

        def other(k, start, size):
            return others[pl.ds(k * 2 * rows + start, size), :]

        def put(low, high):
            for w, out in enumerate(outs):
                out[pl.ds(0, rows), :] = own_ref[pl.ds(w * rows, rows), :]
                for k in range(1, steps):
                    out[pl.ds(k * rows, rows), :] = high(k - 1, w * rows, rows)
                    out[pl.ds((count - k) * rows, rows), :] = low(k - 1, w * rows, rows)
                out[pl.ds(steps * rows, part), :] = low(steps - 1, w * part, part)
                out[pl.ds(steps * rows + part, part), :] = high(steps - 1, w * part, part)

        pl.when(where_ref[2] == 0)(lambda: put(mine, other))
        pl.when(where_ref[2] == 1)(lambda: put(other, mine))

    unit = jax.ShapeDtypeStruct((count * rows, own.shape[1]), own.dtype)
    size = 2 * (own.size * (count + 1) * 2)
    cost = pl.CostEstimate(flops=1 << 20, bytes_accessed=size, transcendentals=0)
    return vmem_call(
        body, [unit, unit], [where, own, *pieces, theirs], limit=size + (1 << 20), scalars=1, cost_estimate=cost
    )


CHUNK = 64


def by_units(z, y):
    return z * NY + y


EARLY = 14
LATE = NZ * NY - EARLY


def by_arrival(z, y):
    near = (z < 3) | (z > 5)
    order = z - 3 * jnp.where(z > 5, 1, 0)
    low = jnp.where(near, 2 * order + y, EARLY + 12 + 2 * (z - 3) + y)
    side = jnp.where(near & (z != 0), 10 + order - 1, EARLY + 8 + jnp.where(z == 0, 0, z - 2))
    return jnp.where(y < 2, low, jnp.where(y == 2, EARLY + z, side))


def gather(where_ref, out, own, mine, theirs, spread, chunk_of=by_units, first=0, column=0):
    core, steps = where_ref[2], len(mine)
    count = 2 * steps
    chunks = NZ * NY // count
    width = own.shape[1]

    def copy(src, start, unit, offset, size):
        def step(q, _):
            z, y = (offset + q, unit) if spread else (unit, offset + q)
            to = (chunk_of(z, y) - first) * CHUNK

            def move():
                there = pl.ds(pl.multiple_of(to, CHUNK), CHUNK)
                out[there, pl.ds(column, width)] = src[pl.ds(pl.multiple_of(start + q * CHUNK, CHUNK), CHUNK), :]

            if chunk_of is by_units:
                move()
            else:
                pl.when((to >= 0) & (to < out.shape[0]))(move)
            return 0

        lax.fori_loop(0, size, step, 0)

    copy(own, 0, 0, 0, chunks)
    for k in range(1, steps):
        if mine[k - 1] is not None:
            copy(*mine[k - 1], k + (1 - core) * (count - 2 * k), 0, chunks)
            copy(*theirs[k - 1], k + core * (count - 2 * k), 0, chunks)
    if mine[-1] is not None:
        half = chunks // 2
        copy(*mine[-1], steps, core * half, half)
        copy(*theirs[-1], steps, (1 - core) * half, half)


def gathered(where, sides, first, count):
    def body(where_ref, *refs):
        out, at, column = refs[-1], 0, 0
        for pieces, mine, theirs, spread in sides:
            own = refs[at : at + len(pieces)]
            mine, theirs = ([None if e is None else (own[e[0]], e[1]) for e in es] for es in (mine, theirs))
            gather(where_ref, out, own[0], mine, theirs, spread, by_arrival, first, column)
            at, column = at + len(pieces), column + pieces[0].shape[1]

    pieces = [p for side in sides for p in side[0]]
    out = jax.ShapeDtypeStruct((count * CHUNK, sum(side[0][0].shape[1] for side in sides)), pieces[0].dtype)
    cost = pl.CostEstimate(flops=1 << 20, bytes_accessed=4 * out.size, transcendentals=0)
    return vmem_call(body, out, [where, *pieces], limit=16 << 20, scalars=1, cost_estimate=cost)


def hidden_units(where, tokens, pieces, mine, theirs, spread):
    count, block = len(tokens), tokens[0].shape[0]
    step = 512

    def body(where_ref, *refs):
        refs, (out, all_ref, w_ref) = refs[:-3], refs[-3:]
        for k in range(count):
            all_ref[pl.ds(k * block, block), :] = refs[k][...]
        own = refs[count:]
        gather(where_ref, w_ref, own[0], [(own[i], r) for i, r in mine], [(own[i], r) for i, r in theirs], spread)

        def tile(j, _):
            cols = pl.ds(pl.multiple_of(j * step, step), step)
            pre = jnp.dot(all_ref[...], w_ref[:, cols], preferred_element_type=jnp.float32)
            out[:, cols] = jnp.square(jnp.maximum(pre, 0.0)).astype(jnp.bfloat16)
            return 0

        lax.fori_loop(0, out.shape[1] // step, tile, 0)

    width, units = tokens[0].shape[1], pieces[0].shape[1]
    out = jax.ShapeDtypeStruct((count * block, units), jnp.bfloat16)
    scratch = [pltpu.VMEM((count * block, width), jnp.bfloat16), pltpu.VMEM((width, units), jnp.bfloat16)]
    cost = pl.CostEstimate(flops=2 * out.size * width, bytes_accessed=8 << 20, transcendentals=0)
    args = [where, *tokens, *pieces]
    return vmem_call(body, out, args, limit=16 << 20, scalars=1, cost_estimate=cost, scratch_shapes=scratch)


def layer(tokens, pre_gain, w_expand, w_reduce, post_gain):
    z, y, core = place()
    first = core == 0
    where = jnp.stack([z, y, core]).astype(jnp.int32)

    def low_high(mine, theirs):
        return jnp.where(first, mine, theirs), jnp.where(first, theirs, mine)

    def half(a):
        n = a.shape[0] // 2
        return jnp.where(first, a[:n], a[n:])

    def half_pair(a):
        n = a.shape[0] // 4
        return jnp.concatenate([jnp.where(first, a[k : k + n], a[k + n : k + 2 * n]) for k in (0, 2 * n)], 0)

    mine = jnp.concatenate([w_expand, w_reduce.T], 0)
    other = swap(mine)
    normed = pre_norm(where, tokens, pre_gain)
    block0, block1 = low_high(mine, other)
    z1, z2 = send_z(block0, 1), send_z(block0, 2)
    y1, y2 = send_y(block1, 1), send_y(half_pair(block1), 2)
    everyone = [normed, send_x(normed, -1), send_x(normed, 2), send_x(normed, 1)]
    ys = swap(jnp.concatenate([y1, y2], 0))
    ve, vr = ring_units(where, block1, [y1, y2], ys)
    z3, z4 = send_z(z2, 1), send_z(half_pair(z2), 2)
    zs = swap(jnp.concatenate([z1, z2, z3, z4], 0))
    ue, ur = ring_units(where, block0, [z1, z2, z3, z4], zs)

    def heavy_z(unit):
        v, got = unit, []
        for k in range(4):
            v = send_z(half(v) if k == 3 else v, 1)
            got.append(v)
        return got, swap(jnp.concatenate(got[2:], 0))

    def heavy_y(unit):
        u1 = send_y(unit, 1)
        return u1, send_y(half(u1), 1)

    (ge, se), (gr, sr) = heavy_z(ve), heavy_z(vr)
    near = swap(jnp.concatenate(ge[:2] + gr[:2], 0))
    rows = ve.shape[0]
    ye, yr = heavy_y(ue), heavy_y(ur)
    se1, se2 = swap(ye[0]), swap(ye[1])
    sr1, sr2 = swap(yr[0]), swap(yr[1])
    by_z = [(k, 0) for k in (1, 2, 3, 4)]
    by_y = [(k, 0) for k in (1, 2)]
    theirs = [(3, 0), (4, 0)]
    h0 = hidden_units(where, everyone, [ue, *ye, se1, se2], by_y, theirs, True)
    theirs = [(5, 0), (5, rows), (6, 0), (6, rows)]
    h1 = hidden_units(where, everyone, [ve, *ge, near, se], by_z, theirs, False)
    theirs = [(5, 2 * rows), (5, 3 * rows), (6, 0), (6, rows)]
    hidden = jnp.concatenate([h0, h1], 1)
    late0 = ([ur, *yr, sr1, sr2], by_y, [(3, 0), (4, 0)], True)
    late1 = ([vr, *gr, near, sr], by_z, theirs, False)
    early0 = ([ur, yr[0], sr1], [(1, 0), None], [(2, 0), None], True)
    early1 = ([vr, gr[0], gr[1], near], [(1, 0), (2, 0), None, None], [(3, 2 * rows), (3, 3 * rows), None, None], False)
    parts = []
    tn = (((1,), (1,)), ((), ()))
    rows = tokens.shape[0]
    for sides, first, count in (((early0, early1), 0, EARLY), ((late0, late1), EARLY, LATE)):
        w = gathered(where, sides, first, count)
        mixed = lax.dot_general(hidden, w, tn, preferred_element_type=jnp.float32).astype(jnp.bfloat16)
        m = [mixed[k * rows : (k + 1) * rows] for k in range(NX)]
        got = [send_x(m[k], k if k < 3 else -1) for k in (2, 3, 1)]
        parts.append([m[0], *got])
    return last_norm(where, parts, post_gain)


def solution(mesh):
    return jax.shard_map(
        layer,
        mesh=mesh,
        in_specs=(P(("fs", "tp"), None), P(), P("fs", "tp"), P("tp", "fs"), P()),
        out_specs=P(("fs", "tp"), None),
        check_vma=False,
    )
```

```python
import jax
import jax.numpy as jnp
from jax import lax
from jax.experimental import pallas as pl
from jax.experimental.pallas import tpu as pltpu
from jax.sharding import PartitionSpec as P

NORM_EPS = 1e-06
NZ, NY, NX = 8, 4, 4
AXES = ("fs", "tp")


def flat(z, y, x, c):
    return ((z % NZ) * NY + y % NY) * (2 * NX) + (x % NX) * 2 + c


def moves(step):
    return [
        (flat(z, y, x, c), flat(*step(z, y, x, c)))
        for z in range(NZ)
        for y in range(NY)
        for x in range(NX)
        for c in range(2)
    ]


def send_z(a, d):
    return lax.ppermute(a, AXES, moves(lambda z, y, x, c: (z + (d if c == 0 else -d), y, x, c)))


def send_y(a, d):
    return lax.ppermute(a, AXES, moves(lambda z, y, x, c: (z, y + (d if c == 0 else -d), x, c)))


def send_x(a, d):
    return lax.ppermute(a, AXES, moves(lambda z, y, x, c: (z, y, x + d, c)))


def swap(a):
    return lax.ppermute(a, AXES, moves(lambda z, y, x, c: (z, y, x, 1 - c)))


def place():
    fs, tp = lax.axis_index("fs"), lax.axis_index("tp")
    return fs // NY, fs % NY, tp % 2


ROWS = 16
UNIT = 256


def unit_at(k):
    return pl.ds(pl.multiple_of(lax.rem(k, NZ) * UNIT, UNIT), UNIT)


def norm_body(where_ref, x_ref, gain_ref, out_ref):
    def step(i, _):
        rows = pl.ds(pl.multiple_of(i * ROWS, ROWS), ROWS)
        x = x_ref[rows, :].astype(jnp.float32)
        scale = lax.rsqrt(jnp.mean(x * x, axis=-1, keepdims=True) + NORM_EPS)
        y = (x * scale) * gain_ref[...]
        turn = lax.rem(NY - where_ref[1], NY) * (UNIT // NY)
        for k in range(NZ):
            unit = pltpu.roll(y[:, UNIT * k : UNIT * (k + 1)], turn, 1)
            out_ref[rows, unit_at(k + NZ - where_ref[0])] = unit.astype(jnp.bfloat16)
        return 0

    lax.fori_loop(0, x_ref.shape[0] // ROWS, step, 0)


def pre_norm(where, tokens, gain):
    cost = pl.CostEstimate(flops=8 << 20, bytes_accessed=1 << 20, transcendentals=128)
    out = jax.ShapeDtypeStruct(tokens.shape, jnp.bfloat16)
    args = [where, tokens, gain.reshape(1, -1)]
    return vmem_call(norm_body, out, args, limit=4 << 20, scalars=1, cost_estimate=cost)


def total_of(parts, rows):
    total = parts[0][rows, :].astype(jnp.float32)
    for p in parts[1:]:
        total += p[rows, :].astype(jnp.float32)
    return total.astype(jnp.bfloat16)


def added(parts):
    def body(*refs):
        def step(i, _):
            rows = pl.ds(pl.multiple_of(i * ROWS, ROWS), ROWS)
            refs[-1][rows, :] = total_of(refs[:-1], rows)
            return 0

        lax.fori_loop(0, refs[-1].shape[0] // ROWS, step, 0)

    out = jax.ShapeDtypeStruct(parts[0].shape, parts[0].dtype)
    cost = pl.CostEstimate(flops=out.size, bytes_accessed=2 * out.size, transcendentals=0)
    return vmem_call(body, out, parts, limit=4 << 20, cost_estimate=cost)


def last_body(sizes, where_ref, *refs):
    parts, gain_ref, out_ref = refs[:-2], refs[-2], refs[-1]
    block = 4 * ROWS

    def step(i, _):
        rows = pl.ds(pl.multiple_of(i * block, block), block)
        sums, at = [], 0
        for size in sizes:
            sums.append(total_of(parts[at : at + size], rows).astype(jnp.float32))
            at += size
        square = sum(jnp.sum(x * x, axis=-1, keepdims=True) for x in sums)
        scale = lax.rsqrt(square / out_ref.shape[1] + NORM_EPS)
        x = jnp.concatenate(sums, axis=1) * scale

        def cut(z, y, n=1):
            at = CHUNK * chunk_at(z, y)
            return x[:, at : at + n * CHUNK]

        turn = where_ref[1] * (UNIT // NY)
        for k in range(NZ):
            unit = jnp.concatenate([cut(k, 0, 2), cut(k, 2), cut(k, 3)], axis=1)
            unit = pltpu.roll(unit, turn, 1)
            there = unit_at(k + where_ref[0])
            out_ref[rows, there] = (unit * gain_ref[:, there]).astype(jnp.bfloat16)
        return 0

    lax.fori_loop(0, out_ref.shape[0] // block, step, 0)


def chunk_at(z, y):
    near = z < 3 or z > 5
    order = z - 3 if z > 5 else z
    if y < 2:
        return 2 * order + y if near else EARLY + 12 + 2 * (z - 3) + y
    if y == 2:
        return EARLY + z
    return 10 + order - 1 if near and z != 0 else EARLY + 8 + (z - 2 if z else 0)


def last_norm(where, groups, gain):
    parts = [p for g in groups for p in g]
    out = jax.ShapeDtypeStruct((parts[0].shape[0], gain.shape[0]), jnp.bfloat16)

    def body(*refs):
        last_body([len(g) for g in groups], *refs)

    args = [where, *parts, gain.reshape(1, -1)]
    return vmem_call(body, out, args, limit=6 << 20, scalars=1)


def vmem_call(body, outs, args, limit, scalars=0, **kw):
    return pl.pallas_call(
        body,
        out_shape=outs,
        in_specs=[pl.BlockSpec(memory_space=pltpu.SMEM)] * scalars
        + [pl.BlockSpec(memory_space=pltpu.VMEM)] * (len(args) - scalars),
        out_specs=jax.tree.map(lambda _: pl.BlockSpec(memory_space=pltpu.VMEM), outs),
        compiler_params=pltpu.CompilerParams(vmem_limit_bytes=limit),
        **kw,
    )(*args)


def ring_units(where, own, pieces, theirs):
    steps = len(pieces)
    count, rows = 2 * steps, own.shape[0] // 2
    part = rows // 2

    def body(where_ref, own_ref, *refs):
        others, outs = refs[steps], refs[steps + 1 :]

        def mine(k, start, size):
            return refs[k][pl.ds(start, size), :]

        def other(k, start, size):
            return others[pl.ds(k * 2 * rows + start, size), :]

        def put(low, high):
            for w, out in enumerate(outs):
                out[pl.ds(0, rows), :] = own_ref[pl.ds(w * rows, rows), :]
                for k in range(1, steps):
                    out[pl.ds(k * rows, rows), :] = high(k - 1, w * rows, rows)
                    out[pl.ds((count - k) * rows, rows), :] = low(k - 1, w * rows, rows)
                out[pl.ds(steps * rows, part), :] = low(steps - 1, w * part, part)
                out[pl.ds(steps * rows + part, part), :] = high(steps - 1, w * part, part)

        pl.when(where_ref[2] == 0)(lambda: put(mine, other))
        pl.when(where_ref[2] == 1)(lambda: put(other, mine))

    unit = jax.ShapeDtypeStruct((count * rows, own.shape[1]), own.dtype)
    size = 2 * (own.size * (count + 1) * 2)
    cost = pl.CostEstimate(flops=1 << 20, bytes_accessed=size, transcendentals=0)
    return vmem_call(
        body, [unit, unit], [where, own, *pieces, theirs], limit=size + (1 << 20), scalars=1, cost_estimate=cost
    )


CHUNK = 64


def by_units(z, y):
    return z * NY + y


EARLY = 14
LATE = NZ * NY - EARLY


def by_arrival(z, y):
    near = (z < 3) | (z > 5)
    order = z - 3 * jnp.where(z > 5, 1, 0)
    low = jnp.where(near, 2 * order + y, EARLY + 12 + 2 * (z - 3) + y)
    side = jnp.where(near & (z != 0), 10 + order - 1, EARLY + 8 + jnp.where(z == 0, 0, z - 2))
    return jnp.where(y < 2, low, jnp.where(y == 2, EARLY + z, side))


def is_early(k, q, spread):
    if not spread:
        return k < 3 and (q < 2 or (q == 3 and k != 0))
    if k == 2 or 3 <= q <= 5:
        return False
    return None if k == 1 and q == 0 else True


def gather(where_ref, out, own, mine, theirs, spread, chunk_of=by_units, first=0, column=0):
    core, steps = where_ref[2], len(mine)
    count = 2 * steps
    chunks = NZ * NY // count
    width = own.shape[1]

    def copy(src, start, k, unit, offset, size):
        for q in range(size):
            z, y = (offset + q, unit) if spread else (unit, offset + q)
            to = (chunk_of(z, y) - first) * CHUNK

            def move(to=to, q=q):
                there = pl.ds(pl.multiple_of(to, CHUNK), CHUNK)
                out[there, pl.ds(column, width)] = src[pl.ds(start + q * CHUNK, CHUNK), :]

            early = is_early(k, q, spread)
            if chunk_of is by_units or early is (first == 0):
                move()
            elif early is None:
                pl.when((to >= 0) & (to < out.shape[0]))(move)

    copy(own, 0, 0, 0 * core, 0, chunks)
    for k in range(1, steps):
        if mine[k - 1] is not None:
            copy(*mine[k - 1], k, k + (1 - core) * (count - 2 * k), 0, chunks)
            copy(*theirs[k - 1], k, k + core * (count - 2 * k), 0, chunks)
    if mine[-1] is not None:
        half = chunks // 2
        copy(*mine[-1], steps, steps + 0 * core, core * half, half)
        copy(*theirs[-1], steps, steps + 0 * core, (1 - core) * half, half)


def gathered(where, sides, first, count):
    def body(where_ref, *refs):
        out, at, column = refs[-1], 0, 0
        for pieces, mine, theirs, spread in sides:
            own = refs[at : at + len(pieces)]
            mine, theirs = ([None if e is None else (own[e[0]], e[1]) for e in es] for es in (mine, theirs))
            gather(where_ref, out, own[0], mine, theirs, spread, by_arrival, first, column)
            at, column = at + len(pieces), column + pieces[0].shape[1]

    pieces = [p for side in sides for p in side[0]]
    out = jax.ShapeDtypeStruct((count * CHUNK, sum(side[0][0].shape[1] for side in sides)), pieces[0].dtype)
    cost = pl.CostEstimate(flops=1 << 20, bytes_accessed=4 * out.size, transcendentals=0)
    return vmem_call(body, out, [where, *pieces], limit=16 << 20, scalars=1, cost_estimate=cost)


def hidden_units(where, tokens, pieces, mine, theirs, spread):
    count, block = len(tokens), tokens[0].shape[0]
    step = 512

    def body(where_ref, *refs):
        if count > 1:
            refs, (out, all_ref, w_ref) = refs[:-3], refs[-3:]
            for k in range(count):
                all_ref[pl.ds(k * block, block), :] = refs[k][...]
        else:
            refs, (out, w_ref), all_ref = refs[:-2], refs[-2:], refs[0]
        own = refs[count:]
        gather(where_ref, w_ref, own[0], [(own[i], r) for i, r in mine], [(own[i], r) for i, r in theirs], spread)

        def tile(j, _):
            cols = pl.ds(pl.multiple_of(j * step, step), step)
            pre = jnp.dot(all_ref[...], w_ref[:, cols], preferred_element_type=jnp.float32)
            out[:, cols] = jnp.square(jnp.maximum(pre, 0.0)).astype(jnp.bfloat16)
            return 0

        lax.fori_loop(0, out.shape[1] // step, tile, 0)

    width, units = tokens[0].shape[1], pieces[0].shape[1]
    out = jax.ShapeDtypeStruct((count * block, units), jnp.bfloat16)
    outs = [out] + [jax.ShapeDtypeStruct((count * block, width), jnp.bfloat16)] * (count > 1)
    scratch = [pltpu.VMEM((width, units), jnp.bfloat16)]
    cost = pl.CostEstimate(flops=2 * out.size * width, bytes_accessed=8 << 20, transcendentals=0)
    args = [where, *tokens, *pieces]
    return vmem_call(body, outs, args, limit=16 << 20, scalars=1, cost_estimate=cost, scratch_shapes=scratch)


def layer(tokens, pre_gain, w_expand, w_reduce, post_gain):
    z, y, core = place()
    first = core == 0
    where = jnp.stack([z, y, core]).astype(jnp.int32)

    def low_high(mine, theirs):
        return jnp.where(first, mine, theirs), jnp.where(first, theirs, mine)

    def half(a):
        n = a.shape[0] // 2
        return jnp.where(first, a[:n], a[n:])

    def half_pair(a):
        n = a.shape[0] // 4
        return jnp.concatenate([jnp.where(first, a[k : k + n], a[k + n : k + 2 * n]) for k in (0, 2 * n)], 0)

    mine = jnp.concatenate([w_expand, w_reduce.T], 0)
    other = swap(mine)
    normed = pre_norm(where, tokens, pre_gain)
    block0, block1 = low_high(mine, other)
    z1, z2 = send_z(block0, 1), send_z(block0, 2)
    y1, y2 = send_y(block1, 1), send_y(half_pair(block1), 2)
    everyone = [normed, send_x(normed, -1), send_x(normed, 2), send_x(normed, 1)]
    ys = swap(jnp.concatenate([y1, y2], 0))
    ve, vr = ring_units(where, block1, [y1, y2], ys)
    z3, z4 = send_z(z2, 1), send_z(half_pair(z2), 2)
    zs = swap(jnp.concatenate([z1, z2, z3, z4], 0))
    ue, ur = ring_units(where, block0, [z1, z2, z3, z4], zs)

    def heavy_z(unit):
        v, got = unit, []
        for k in range(4):
            v = send_z(half(v) if k == 3 else v, 1)
            got.append(v)
        return got, swap(jnp.concatenate(got[2:], 0))

    def heavy_y(unit):
        u1 = send_y(unit, 1)
        return u1, send_y(half(u1), 1)

    (ge, se), (gr, sr) = heavy_z(ve), heavy_z(vr)
    near = swap(jnp.concatenate(ge[:2] + gr[:2], 0))
    rows = ve.shape[0]
    ye, yr = heavy_y(ue), heavy_y(ur)
    se1, se2 = swap(ye[0]), swap(ye[1])
    sr1, sr2 = swap(yr[0]), swap(yr[1])
    by_z = [(k, 0) for k in (1, 2, 3, 4)]
    by_y = [(k, 0) for k in (1, 2)]
    theirs = [(3, 0), (4, 0)]
    h0, everyone = hidden_units(where, everyone, [ue, *ye, se1, se2], by_y, theirs, True)
    theirs = [(5, 0), (5, rows), (6, 0), (6, rows)]
    (h1,) = hidden_units(where, [everyone], [ve, *ge, near, se], by_z, theirs, False)
    theirs = [(5, 2 * rows), (5, 3 * rows), (6, 0), (6, rows)]
    hidden = jnp.concatenate([h0, h1], 1)
    late0 = ([ur, *yr, sr1, sr2], by_y, [(3, 0), (4, 0)], True)
    late1 = ([vr, *gr, near, sr], by_z, theirs, False)
    early0 = ([ur, yr[0], sr1], [(1, 0), None], [(2, 0), None], True)
    early1 = ([vr, gr[0], gr[1], near], [(1, 0), (2, 0), None, None], [(3, 2 * rows), (3, 3 * rows), None, None], False)
    parts = []
    tn = (((1,), (1,)), ((), ()))
    rows = tokens.shape[0]
    for g, sides, first, count in (("A", (early0, early1), 0, EARLY), ("B", (late0, late1), EARLY, LATE)):
        w = gathered(where, sides, first, count)

        def mix(a):
            return lax.dot_general(a, w, tn, preferred_element_type=jnp.float32).astype(jnp.bfloat16)

        if g == "A":
            near, far = mix(hidden[: 2 * rows]), mix(hidden[2 * rows :])
            m = [near[:rows], near[rows:], far[:rows], far[rows:]]
        else:
            mixed = mix(hidden)
            m = [mixed[k * rows : (k + 1) * rows] for k in range(NX)]
        got = [send_x(m[k], k if k < 3 else -1) for k in (2, 3, 1)]
        parts.append([m[0], *got] if g == "B" else [added([m[0], *got])])
    return last_norm(where, parts, post_gain)


def solution(mesh):
    return jax.shard_map(
        layer,
        mesh=mesh,
        in_specs=(P(("fs", "tp"), None), P(), P("fs", "tp"), P("tp", "fs"), P()),
        out_specs=P(("fs", "tp"), None),
        check_vma=False,
    )
```

```python
import jax
import jax.numpy as jnp
from jax import lax
from jax.experimental import pallas as pl
from jax.experimental.pallas import tpu as pltpu
from jax.sharding import PartitionSpec as P

NORM_EPS = 1e-06
NZ, NY, NX = 8, 4, 4
AXES = ("fs", "tp")


def flat(z, y, x, c):
    return ((z % NZ) * NY + y % NY) * (2 * NX) + (x % NX) * 2 + c


def moves(step):
    return [
        (flat(z, y, x, c), flat(*step(z, y, x, c)))
        for z in range(NZ)
        for y in range(NY)
        for x in range(NX)
        for c in range(2)
    ]


def send_z(a, d):
    return lax.ppermute(a, AXES, moves(lambda z, y, x, c: (z + (d if c == 0 else -d), y, x, c)))


def send_y(a, d):
    return lax.ppermute(a, AXES, moves(lambda z, y, x, c: (z, y + (d if c == 0 else -d), x, c)))


def send_x(a, d):
    return lax.ppermute(a, AXES, moves(lambda z, y, x, c: (z, y, x + d, c)))


def swap(a):
    return lax.ppermute(a, AXES, moves(lambda z, y, x, c: (z, y, x, 1 - c)))


def place():
    fs, tp = lax.axis_index("fs"), lax.axis_index("tp")
    return fs // NY, fs % NY, tp % 2


ROWS = 16
UNIT = 256


def unit_at(k):
    return pl.ds(pl.multiple_of(lax.rem(k, NZ) * UNIT, UNIT), UNIT)


def norm_body(where_ref, x_ref, gain_ref, out_ref):
    def step(i, _):
        rows = pl.ds(pl.multiple_of(i * ROWS, ROWS), ROWS)
        x = x_ref[rows, :].astype(jnp.float32)
        scale = lax.rsqrt(jnp.mean(x * x, axis=-1, keepdims=True) + NORM_EPS)
        y = (x * scale) * gain_ref[...]
        turn = lax.rem(NY - where_ref[1], NY) * (UNIT // NY)
        for k in range(NZ):
            unit = pltpu.roll(y[:, UNIT * k : UNIT * (k + 1)], turn, 1)
            out_ref[rows, unit_at(k + NZ - where_ref[0])] = unit.astype(jnp.bfloat16)
        return 0

    lax.fori_loop(0, x_ref.shape[0] // ROWS, step, 0)


def pre_norm(where, tokens, gain):
    cost = pl.CostEstimate(flops=8 << 20, bytes_accessed=1 << 20, transcendentals=128)
    out = jax.ShapeDtypeStruct(tokens.shape, jnp.bfloat16)
    args = [where, tokens, gain.reshape(1, -1)]
    return vmem_call(norm_body, out, args, limit=4 << 20, scalars=1, cost_estimate=cost)


def total_of(parts, rows):
    total = parts[0][rows, :].astype(jnp.float32)
    for p in parts[1:]:
        total += p[rows, :].astype(jnp.float32)
    return total.astype(jnp.bfloat16)


def added(parts):
    def body(*refs):
        def step(i, _):
            rows = pl.ds(pl.multiple_of(i * ROWS, ROWS), ROWS)
            refs[-1][rows, :] = total_of(refs[:-1], rows)
            return 0

        lax.fori_loop(0, refs[-1].shape[0] // ROWS, step, 0)

    out = jax.ShapeDtypeStruct(parts[0].shape, parts[0].dtype)
    cost = pl.CostEstimate(flops=out.size, bytes_accessed=2 * out.size, transcendentals=0)
    return vmem_call(body, out, parts, limit=4 << 20, cost_estimate=cost)


def last_body(sizes, where_ref, *refs):
    parts, gain_ref, out_ref = refs[:-2], refs[-2], refs[-1]
    block = 4 * ROWS

    def step(i, _):
        rows = pl.ds(pl.multiple_of(i * block, block), block)
        sums, at = [], 0
        for size in sizes:
            sums.append(total_of(parts[at : at + size], rows).astype(jnp.float32))
            at += size
        square = sum(jnp.sum(x * x, axis=-1, keepdims=True) for x in sums)
        scale = lax.rsqrt(square / out_ref.shape[1] + NORM_EPS)
        x = jnp.concatenate(sums, axis=1) * scale

        def cut(z, y, n=1):
            at = CHUNK * chunk_at(z, y)
            return x[:, at : at + n * CHUNK]

        turn = where_ref[1] * (UNIT // NY)
        for k in range(NZ):
            unit = jnp.concatenate([cut(k, 0, 2), cut(k, 2), cut(k, 3)], axis=1)
            unit = pltpu.roll(unit, turn, 1)
            there = unit_at(k + where_ref[0])
            out_ref[rows, there] = (unit * gain_ref[:, there]).astype(jnp.bfloat16)
        return 0

    lax.fori_loop(0, out_ref.shape[0] // block, step, 0)


def chunk_at(z, y):
    near = z < 3 or z > 5
    order = z - 3 if z > 5 else z
    if y < 2:
        return 2 * order + y if near else EARLY + 12 + 2 * (z - 3) + y
    if y == 2:
        return EARLY + z
    return 10 + order - 1 if near and z != 0 else EARLY + 8 + (z - 2 if z else 0)


def last_norm(where, groups, gain):
    parts = [p for g in groups for p in g]
    out = jax.ShapeDtypeStruct((parts[0].shape[0], gain.shape[0]), jnp.bfloat16)

    def body(*refs):
        last_body([len(g) for g in groups], *refs)

    args = [where, *parts, gain.reshape(1, -1)]
    return vmem_call(body, out, args, limit=6 << 20, scalars=1)


def vmem_call(body, outs, args, limit, scalars=0, **kw):
    return pl.pallas_call(
        body,
        out_shape=outs,
        in_specs=[pl.BlockSpec(memory_space=pltpu.SMEM)] * scalars
        + [pl.BlockSpec(memory_space=pltpu.VMEM)] * (len(args) - scalars),
        out_specs=jax.tree.map(lambda _: pl.BlockSpec(memory_space=pltpu.VMEM), outs),
        compiler_params=pltpu.CompilerParams(vmem_limit_bytes=limit),
        **kw,
    )(*args)


def ring_units(where, own, pieces, theirs):
    steps = len(pieces)
    count, rows = 2 * steps, own.shape[0] // 2
    part = rows // 2

    def body(where_ref, own_ref, *refs):
        others, outs = refs[steps], refs[steps + 1 :]

        def mine(k, start, size):
            return refs[k][pl.ds(start, size), :]

        def other(k, start, size):
            return others[pl.ds(k * 2 * rows + start, size), :]

        def put(low, high):
            for w, out in enumerate(outs):
                out[pl.ds(0, rows), :] = own_ref[pl.ds(w * rows, rows), :]
                for k in range(1, steps):
                    out[pl.ds(k * rows, rows), :] = high(k - 1, w * rows, rows)
                    out[pl.ds((count - k) * rows, rows), :] = low(k - 1, w * rows, rows)
                out[pl.ds(steps * rows, part), :] = low(steps - 1, w * part, part)
                out[pl.ds(steps * rows + part, part), :] = high(steps - 1, w * part, part)

        pl.when(where_ref[2] == 0)(lambda: put(mine, other))
        pl.when(where_ref[2] == 1)(lambda: put(other, mine))

    unit = jax.ShapeDtypeStruct((count * rows, own.shape[1]), own.dtype)
    size = 2 * (own.size * (count + 1) * 2)
    cost = pl.CostEstimate(flops=1 << 20, bytes_accessed=size, transcendentals=0)
    return vmem_call(
        body, [unit, unit], [where, own, *pieces, theirs], limit=size + (1 << 20), scalars=1, cost_estimate=cost
    )


CHUNK = 64


def by_units(z, y):
    return z * NY + y


EARLY = 14
LATE = NZ * NY - EARLY


def by_arrival(z, y):
    near = (z < 3) | (z > 5)
    order = z - 3 * jnp.where(z > 5, 1, 0)
    low = jnp.where(near, 2 * order + y, EARLY + 12 + 2 * (z - 3) + y)
    side = jnp.where(near & (z != 0), 10 + order - 1, EARLY + 8 + jnp.where(z == 0, 0, z - 2))
    return jnp.where(y < 2, low, jnp.where(y == 2, EARLY + z, side))


def is_early(k, q, spread):
    if not spread:
        return k < 3 and (q < 2 or (q == 3 and k != 0))
    if k == 2 or 3 <= q <= 5:
        return False
    return None if k == 1 and q == 0 else True


def gather(where_ref, out, own, mine, theirs, spread, chunk_of=by_units, first=0, column=0):
    core, steps = where_ref[2], len(mine)
    count = 2 * steps
    chunks = NZ * NY // count
    width = own.shape[1]

    def copy(src, start, k, unit, offset, size):
        for q in range(size):
            z, y = (offset + q, unit) if spread else (unit, offset + q)
            to = (chunk_of(z, y) - first) * CHUNK

            def move(to=to, q=q):
                there = pl.ds(pl.multiple_of(to, CHUNK), CHUNK)
                out[there, pl.ds(column, width)] = src[pl.ds(start + q * CHUNK, CHUNK), :]

            early = is_early(k, q, spread)
            if chunk_of is by_units or early is (first == 0):
                move()
            elif early is None:
                pl.when((to >= 0) & (to < out.shape[0]))(move)

    copy(own, 0, 0, 0 * core, 0, chunks)
    for k in range(1, steps):
        if mine[k - 1] is not None:
            copy(*mine[k - 1], k, k + (1 - core) * (count - 2 * k), 0, chunks)
            copy(*theirs[k - 1], k, k + core * (count - 2 * k), 0, chunks)
    if mine[-1] is not None:
        half = chunks // 2
        copy(*mine[-1], steps, steps + 0 * core, core * half, half)
        copy(*theirs[-1], steps, steps + 0 * core, (1 - core) * half, half)


def gathered(where, sides, first, count):
    def body(where_ref, *refs):
        out, at, column = refs[-1], 0, 0
        for pieces, mine, theirs, spread in sides:
            own = refs[at : at + len(pieces)]
            mine, theirs = ([None if e is None else (own[e[0]], e[1]) for e in es] for es in (mine, theirs))
            gather(where_ref, out, own[0], mine, theirs, spread, by_arrival, first, column)
            at, column = at + len(pieces), column + pieces[0].shape[1]

    pieces = [p for side in sides for p in side[0]]
    out = jax.ShapeDtypeStruct((count * CHUNK, sum(side[0][0].shape[1] for side in sides)), pieces[0].dtype)
    cost = pl.CostEstimate(flops=1 << 20, bytes_accessed=4 * out.size, transcendentals=0)
    return vmem_call(body, out, [where, *pieces], limit=16 << 20, scalars=1, cost_estimate=cost)


def hidden_units(where, tokens, pieces, mine, theirs, spread):
    count, block = len(tokens), tokens[0].shape[0]
    step = 512

    def body(where_ref, *refs):
        if count > 1:
            refs, (out, all_ref, w_ref) = refs[:-3], refs[-3:]
            for k in range(count):
                all_ref[pl.ds(k * block, block), :] = refs[k][...]
        else:
            refs, (out, w_ref), all_ref = refs[:-2], refs[-2:], refs[0]
        own = refs[count:]
        gather(where_ref, w_ref, own[0], [(own[i], r) for i, r in mine], [(own[i], r) for i, r in theirs], spread)

        def tile(j, _):
            cols = pl.ds(pl.multiple_of(j * step, step), step)
            pre = jnp.dot(all_ref[...], w_ref[:, cols], preferred_element_type=jnp.float32)
            out[:, cols] = jnp.square(jnp.maximum(pre, 0.0)).astype(jnp.bfloat16)
            return 0

        lax.fori_loop(0, out.shape[1] // step, tile, 0)

    width, units = tokens[0].shape[1], pieces[0].shape[1]
    out = jax.ShapeDtypeStruct((count * block, units), jnp.bfloat16)
    outs = [out] + [jax.ShapeDtypeStruct((count * block, width), jnp.bfloat16)] * (count > 1)
    scratch = [pltpu.VMEM((width, units), jnp.bfloat16)]
    cost = pl.CostEstimate(flops=2 * out.size * width, bytes_accessed=8 << 20, transcendentals=0)
    args = [where, *tokens, *pieces]
    return vmem_call(body, outs, args, limit=16 << 20, scalars=1, cost_estimate=cost, scratch_shapes=scratch)


def by_core(where, mine, other):
    def body(where_ref, mine_ref, other_ref, *outs):
        for core, (a, b) in enumerate(((mine_ref, other_ref), (other_ref, mine_ref))):

            def copy(a=a, b=b):
                outs[0][...] = a[...]
                outs[1][...] = b[...]

            pl.when(where_ref[2] == core)(copy)

    out = jax.ShapeDtypeStruct(mine.shape, mine.dtype)
    cost = pl.CostEstimate(flops=1 << 20, bytes_accessed=8 * out.size, transcendentals=0)
    return vmem_call(body, [out, out], [where, mine, other], limit=3 << 20, scalars=1, cost_estimate=cost)


def layer(tokens, pre_gain, w_expand, w_reduce, post_gain):
    z, y, core = place()
    first = core == 0
    where = jnp.stack([z, y, core]).astype(jnp.int32)

    def half(a):
        n = a.shape[0] // 2
        return jnp.where(first, a[:n], a[n:])

    def half_pair(a):
        n = a.shape[0] // 4
        return jnp.concatenate([jnp.where(first, a[k : k + n], a[k + n : k + 2 * n]) for k in (0, 2 * n)], 0)

    mine = jnp.concatenate([w_expand, w_reduce.T], 0)
    other = swap(mine)
    normed = pre_norm(where, tokens, pre_gain)
    block0, block1 = by_core(where, mine, other)
    z1, z2 = send_z(block0, 1), send_z(block0, 2)
    y1, y2 = send_y(block1, 1), send_y(half_pair(block1), 2)
    everyone = [normed, send_x(normed, -1), send_x(normed, 2), send_x(normed, 1)]
    ys = swap(jnp.concatenate([y1, y2], 0))
    ve, vr = ring_units(where, block1, [y1, y2], ys)
    z3, z4 = send_z(z2, 1), send_z(half_pair(z2), 2)
    zs = swap(jnp.concatenate([z1, z2, z3, z4], 0))
    ue, ur = ring_units(where, block0, [z1, z2, z3, z4], zs)

    def heavy_z(unit):
        v, got = unit, []
        for k in range(4):
            v = send_z(half(v) if k == 3 else v, 1)
            got.append(v)
        return got, swap(jnp.concatenate(got[2:], 0))

    def heavy_y(unit):
        u1 = send_y(unit, 1)
        return u1, send_y(half(u1), 1)

    (ge, se), (gr, sr) = heavy_z(ve), heavy_z(vr)
    near = swap(jnp.concatenate(ge[:2] + gr[:2], 0))
    rows = ve.shape[0]
    ye, yr = heavy_y(ue), heavy_y(ur)
    se1, se2 = swap(ye[0]), swap(ye[1])
    sr1, sr2 = swap(yr[0]), swap(yr[1])
    by_z = [(k, 0) for k in (1, 2, 3, 4)]
    by_y = [(k, 0) for k in (1, 2)]
    theirs = [(5, 0), (5, rows), (6, 0), (6, rows)]
    h1, everyone = hidden_units(where, everyone, [ve, *ge, near, se], by_z, theirs, False)
    theirs = [(3, 0), (4, 0)]
    (h0,) = hidden_units(where, [everyone], [ue, *ye, se1, se2], by_y, theirs, True)
    theirs = [(5, 2 * rows), (5, 3 * rows), (6, 0), (6, rows)]
    hidden = jnp.concatenate([h0, h1], 1)
    late0 = ([ur, *yr, sr1, sr2], by_y, [(3, 0), (4, 0)], True)
    late1 = ([vr, *gr, near, sr], by_z, theirs, False)
    early0 = ([ur, yr[0], sr1], [(1, 0), None], [(2, 0), None], True)
    early1 = ([vr, gr[0], gr[1], near], [(1, 0), (2, 0), None, None], [(3, 2 * rows), (3, 3 * rows), None, None], False)
    parts = []
    tn = (((1,), (1,)), ((), ()))
    rows = tokens.shape[0]
    for g, sides, first, count in (("A", (early0, early1), 0, EARLY), ("B", (late0, late1), EARLY, LATE)):
        w = gathered(where, sides, first, count)

        def mix(a):
            return lax.dot_general(a, w, tn, preferred_element_type=jnp.float32).astype(jnp.bfloat16)

        near, far = mix(hidden[: 2 * rows]), mix(hidden[2 * rows :])
        m = [near[:rows], near[rows:], far[:rows], far[rows:]]
        got = [send_x(m[k], k if k < 3 else -1) for k in (2, 3, 1)]
        parts.append([m[0], *got] if g == "B" else [added([m[0], *got])])
    return last_norm(where, parts, post_gain)


def solution(mesh):
    return jax.shard_map(
        layer,
        mesh=mesh,
        in_specs=(P(("fs", "tp"), None), P(), P("fs", "tp"), P("tp", "fs"), P()),
        out_specs=P(("fs", "tp"), None),
        check_vma=False,
    )
```
